32 devices in a mesh: fs: 4 (over y, x), tp: 8 (over z, core).
Axes of the slice: x: 2, y: 2, z: 4, core: 2. Of those that a mesh axis runs over, the one named last changes fastest.
Arguments:
- tokens: bfloat16 [4096, 2048], P(('fs', 'tp')), may hold values from -6 to 6
- norm_gain: float32 [2048], P('fs'), may hold values from 0.1 to 1.9
- gate_master: float32 [2048, 8192], P('fs', 'tp'), may hold values from -0.125 to 0.125
- up_master: float32 [2048, 8192], P('fs', 'tp'), may hold values from -0.125 to 0.125
- down_master: float32 [2048, 8192], P('fs', 'tp'), may hold values from -0.09375 to 0.09375
Outputs:
- mixed: bfloat16 [4096, 2048], P(('fs', 'tp'))
- gate_ready: bfloat16 [2048, 8192], P(None, 'tp')
- up_ready: bfloat16 [2048, 8192], P(None, 'tp')
- down_ready: bfloat16 [2048, 8192], P(None, 'tp')
The draws below stay inside these ranges and needn't reach their ends.
All inputs are finite; a program needn't handle non-finite values.
Results may differ from the reference program's by a relative error of at most 0.0095.
Values may be sent and summed in bfloat16 or wider, within the bound.
A program may use at most 64 MiB of HBM per device.

```python
import jax
import jax.numpy as jnp
from jax import lax

D = 2048
FF = 8192
TOKENS = 4096
N_TP = 8


def spiked(drawn, stream_key, source, target, blocks, factor):
    owner, partner = [(jnp.arange(drawn.shape[position]) // (drawn.shape[position] // blocks)).reshape([-1 if axis == position else 1 for axis in range(drawn.ndim)]) for position in (source, target)]
    chosen = jax.random.permutation(stream_key, blocks)[partner]
    strong = (owner == chosen) | (owner == (partner + blocks // 2) % blocks)
    return jnp.where(strong, factor * drawn, drawn)


def level_of(rng, shape, shards, low, high):
    loudness, own = 1.0, jax.random.fold_in(rng, 6)
    for dim, shards_of in shards:
        heights = jnp.exp(jax.random.uniform(jax.random.fold_in(own, dim), (shards_of,), jnp.float32, low / len(shards), high / len(shards)))
        loudness = loudness * jnp.repeat(heights, shape[dim] // shards_of).reshape([-1 if axis == dim else 1 for axis in range(len(shape))])
    return loudness


def centred(key, dims, spread, limit, cuts=(), dtype=jnp.bfloat16):
    drawn = spread * jax.random.normal(key, dims, jnp.float32)
    if cuts:
        drawn = drawn * level_of(key, dims, cuts, -0.22, 0.18)
    return jnp.clip(drawn, -limit, limit).astype(dtype)


def heavy_noise(key, dims, deviation, bound, split, heavy, held_as=jnp.bfloat16):
    drawn = deviation * jax.random.normal(key, dims, jnp.float32)
    if split:
        drawn = drawn * level_of(key, dims, split, -0.22, 0.18)
    return jnp.clip(spiked(drawn, jax.random.fold_in(key, 3), *heavy), -bound, bound).astype(held_as)


def setup_inputs(seed: int = 0) -> dict:
    key_of = jax.random.split(jax.random.key(seed), 6)
    tokens = centred(key_of[0], (TOKENS, D), 1.0, 6.0, ((0, 32),))
    norm_gain = jnp.clip(1.0 + 0.18 * jax.random.normal(key_of[1], (D,), jnp.float32), 0.1, 1.9)
    gate_master = centred(key_of[2], (D, FF), D ** -0.5, 0.125, ((0, 4), (1, 8)), jnp.float32)
    up_master = centred(key_of[3], (D, FF), D ** -0.5, 0.125, ((0, 4), (1, 8)), jnp.float32)
    down_master = heavy_noise(key_of[4], (D, FF), FF ** -0.5, 0.09375, ((0, 4), (1, 8)), (1, 0, 8, 2.0), jnp.float32)
    return {"tokens": tokens, "norm_gain": norm_gain, "gate_master": gate_master, "up_master": up_master, "down_master": down_master}


def reference(tokens, norm_gain, gate_master, up_master, down_master):
    gate_ready = (norm_gain[:, None] * gate_master).astype(jnp.bfloat16)
    up_ready = (norm_gain[:, None] * up_master).astype(jnp.bfloat16)
    down_ready = down_master.astype(jnp.bfloat16)
    tokens_wide = tokens.astype(jnp.float32)
    row_scale = lax.rsqrt(lax.optimization_barrier(jnp.mean(tokens_wide * tokens_wide, axis=1, keepdims=True)) + 1e-06)
    gate_proj = row_scale * jnp.dot(tokens, gate_ready, preferred_element_type=jnp.float32)
    up_proj = row_scale * jnp.dot(tokens, up_ready, preferred_element_type=jnp.float32)
    hidden = (jax.nn.silu(gate_proj) * up_proj).astype(jnp.bfloat16)
    block_width = FF // N_TP
    summed = jnp.zeros((tokens.shape[0], tokens.shape[1]), jnp.float32)
    for column_block in range(N_TP):
        lower = column_block * block_width
        partial_value = lax.dot_general(hidden[:, lower:lower + block_width], down_ready[:, lower:lower + block_width], (((1,), (1,)), ((), ())), preferred_element_type=jnp.float32)
        summed = summed + lax.optimization_barrier(partial_value.astype(jnp.bfloat16)).astype(jnp.float32)
    mixed = (tokens_wide + 0.5 * summed).astype(jnp.bfloat16)
    return (mixed, gate_ready, up_ready, down_ready)
```

```python
import functools
import math

import jax
import jax.numpy as jnp
from jax import lax
from jax.experimental import pallas as pl
from jax.experimental.pallas import tpu as pltpu
from jax.sharding import PartitionSpec as P

MESH = pl.DeviceIdType.MESH
GATE, UP, DOWN = 0, 1, 2


def flip(index, bit):
    return index + bit - 2 * bit * ((index // bit) % 2)


def flip_all(index, mask, dims):
    for dim in range(dims):
        if mask >> dim & 1:
            index = flip(index, 1 << dim)
    return index


def span(bits):
    masks = [0]
    for bit in bits:
        masks += [mask | bit for mask in masks]
    return masks


def plan(n_fs, dims, rows):
    part = rows // dims
    last = n_fs - 1
    if dims != 2 or part % 128 or rows % 256:
        chunks = [([(mask, 0, rows)], [(p, 0, mask) for p in range(dims)], mask) for mask in range(n_fs)]
        return part, part, rows, chunks, last
    chunks = [([(0, at, 256)], [], 0) for at in range(0, rows, 256)]
    for step, owners in enumerate(([(1, 0), (2, 1)], [(2, 0), (1, 1)], [(last, 0), (last, 1)])):
        tall = 64 if step == 2 else 128
        for h in range(part // tall):
            blocks = [(mask, p * part + h * tall, tall) for mask, p in owners]
            chunks.append((blocks, [(p, h, mask) for mask, p in owners], (step, h)))
    return 64, 128, 128, chunks, chunks.index(next(c for c in chunks if c[2] == (1, part // 128 - 1)))


def kernel(
    n_fs, n_z, dims, halves, late_tall, tall_of, width, chunks, first,
    tok_hbm, gain_hbm, gate_hbm, up_hbm, down_hbm,
    mixed, gate, up, down,
    tok_in, gain_row, gain, masters, tok, scale, gate_acc, up_acc, hidden, pair_own, pair_send, pair_recv, z_send, z_pass, z_last,
    w_sent, w_got, t_sent, t_got, s_got, p_sent, p_got, z_sent, z_got, l_got, m_got, loaded,
):
    fs, tp = lax.axis_index("fs"), lax.axis_index("tp")
    z, core = tp // 2, tp % 2
    sibling = z * 2 + 1 - core
    rows, cols = gate_hbm.shape
    part = rows // dims
    own_tok = tok_in.shape[0]
    half = n_z * own_tok
    total = 2 * half
    ready = (gate, up, down)
    every = n_fs - 1

    def cuts(w, mask):
        if w == DOWN:
            return part // (late_tall if mask == every else tall_of)
        return (1, halves)[w]


    loads = {}
    reads = [("gain", gain_hbm, gain_row)]
    for w, master in ((GATE, gate_hbm), (UP, up_hbm)):
        for p in range(dims):
            for i in range(2):
                mine = pl.ds(p * part + i * part // 2, part // 2)
                reads.append(((w, p, i), master.at[mine, :], masters.at[w, mine, :]))
    reads.append(("tok", tok_hbm, tok_in))
    reads.append(("down", down_hbm, masters.at[DOWN]))
    for n, (name, src, dst) in enumerate(reads):
        loads[name] = pltpu.make_async_copy(src, dst, loaded.at[n])

    def z_peer(k):
        return ((z + k) % n_z) * 2 + core

    for name, _, _ in reads[:1 + 2 * dims]:
        loads[name].start()
    barrier = pltpu.get_barrier_semaphore()
    for dim in range(dims):
        pl.semaphore_signal(barrier, 1, device_id={"fs": flip(fs, 1 << dim)}, device_id_type=MESH)
    for k in range(1, n_z):
        pl.semaphore_signal(barrier, 1, device_id={"tp": z_peer(k)}, device_id_type=MESH)
    pl.semaphore_signal(barrier, 1, device_id={"tp": sibling}, device_id_type=MESH)

    loads["gain"].wait()
    for n in range(rows // 128):
        line = gain_row[:, n * 128:(n + 1) * 128]
        gain[n * 128:(n + 1) * 128, :] = jnp.transpose(jnp.broadcast_to(line, (128, 128)))

    def block(w, owner, p, h, mask):
        tall = part // cuts(w, mask)
        start = flip_all(fs, owner, dims) * rows + p * part + h * tall
        return ready[w].at[pl.ds(pl.multiple_of(start, tall), tall), :]

    def order(p):
        return [1 << ((p + s) % dims) for s in range(dims)]

    arrivals = {
        (p, held | order(p)[stage]): stage
        for p in range(dims) for stage in range(dims) for held in span(order(p)[:stage])
    }
    arrived = set()

    place = {}
    for w in (GATE, UP, DOWN):
        for p in range(dims):
            for mask in range(1, n_fs):
                for h in range(cuts(w, mask)):
                    place[w, p, h, mask] = len(place)

    def weight_copy(w, p, h, held, mask, stage):
        return pltpu.make_async_remote_copy(
            src_ref=block(w, held, p, h, mask), dst_ref=block(w, held, p, h, mask),
            send_sem=w_sent.at[w], recv_sem=w_got.at[place[w, p, h, mask]],
            device_id={"fs": flip(fs, order(p)[stage])}, device_id_type=MESH,
        )

    def send(w, p, h, stage, held):
        weight_copy(w, p, h, held, held | order(p)[stage], stage).start()

    def need(w, p, h, mask, hold=False):
        if mask and (w, p, h, mask) not in arrived:
            arrived.add((w, p, h, mask))
            stage = arrivals[p, mask]
            here = block(w, mask, p, h, mask)
            pltpu.make_async_remote_copy(
                src_ref=here, dst_ref=here, send_sem=w_sent.at[w], recv_sem=w_got.at[place[w, p, h, mask]],
                device_id={"fs": flip(fs, order(p)[stage])}, device_id_type=MESH,
            ).wait_recv()
            if not hold:
                forward(w, p, h, mask)

    def forward(w, p, h, mask):
        for later in range(arrivals[p, mask] + 1, dims):
            finer = cuts(w, mask | order(p)[later]) // cuts(w, mask)
            for piece in range(h * finer, (h + 1) * finer):
                send(w, p, piece, later, mask)

    def relays(ws):
        for stage in range(dims - 1):
            for w in ws:
                for p in range(dims):
                    for held in span(order(p)[:stage]):
                        for h in range(cuts(w, held | order(p)[stage])):
                            need(w, p, h, held | order(p)[stage])

    def prepare(w, top, tall):
        mine = slice(top, top + tall)
        value = masters[w, mine, :]
        if w != DOWN:
            value = gain[mine, 0:1] * value
        ready[w][pl.ds(pl.multiple_of(fs * rows + top, tall), tall), :] = value.astype(jnp.bfloat16)

    short = part // 2
    for p in range(dims):
        for i in range(2):
            loads[GATE, p, i].wait()
            prepare(GATE, p * part + i * short, short)
            if p == 0 and i == 0:
                with jax.named_scope("barrier"):
                    pl.semaphore_wait(barrier, dims + n_z)
            at = gate.at[pl.ds(pl.multiple_of(fs * rows + p * part + i * short, short), short), :]
            pltpu.make_async_remote_copy(
                src_ref=at, dst_ref=at, send_sem=w_sent.at[GATE], recv_sem=w_got.at[place[GATE, p, 0, order(p)[0]]],
                device_id={"fs": flip(fs, order(p)[0])}, device_id_type=MESH,
            ).start()
    for name, _, _ in reads[1 + 2 * dims:]:
        loads[name].start()
    for p in range(dims):
        for i in range(2):
            loads[UP, p, i].wait()
        prepare(UP, p * part, part)
        for h in range(cuts(UP, 0)):
            send(UP, p, h, 0, 0)

    def tok_rows(c, chip):
        start = (c * n_z + chip) * own_tok
        return tok.at[pl.ds(pl.multiple_of(start, own_tok), own_tok), :]

    def tok_z(k):
        return pltpu.make_async_remote_copy(
            src_ref=tok_in, dst_ref=tok_rows(core, z), send_sem=t_sent.at[0], recv_sem=t_got.at[k],
            device_id={"tp": z_peer(k)}, device_id_type=MESH,
        )

    def tok_sibling(k, src, slot):
        return pltpu.make_async_remote_copy(
            src_ref=src, dst_ref=slot, send_sem=t_sent.at[0], recv_sem=s_got.at[k],
            device_id={"tp": sibling}, device_id_type=MESH,
        )

    loads["tok"].wait()
    for k in range(1, n_z):
        tok_z(k).start()
    tok_sibling(0, tok_in, tok_rows(core, z)).start()
    for w in (GATE, UP):
        for p in range(dims):
            for stage in range(1, dims):
                for h in range(cuts(w, 0)):
                    send(w, p, h, stage, 0)
    tok_rows(core, z)[...] = tok_in[...]
    loads["down"].wait()
    for p in range(dims):
        prepare(DOWN, p * part, part)

    @pl.when(z == 0)
    def _():
        z_last[0] = jnp.zeros(z_last.shape[1:], jnp.bfloat16)

    @pl.when(z == n_z - 1)
    def _():
        z_last[1] = jnp.zeros(z_last.shape[1:], jnp.bfloat16)

    with jax.named_scope("relays"):
        relays((GATE, UP))

    def send_down(turn, stages):
        @pl.when(core == turn)
        def _():
            for stage in stages:
                for h in range(max(cuts(DOWN, order(p)[stage]) for p in range(dims))):
                    for p in range(dims):
                        send(DOWN, p, h, stage, 0)

    split = dims == 2 and first > 4
    send_down(0, range(1) if split else range(dims))

    for k in range(1, n_z):
        slot = tok_rows(core, (z + n_z - k) % n_z)
        with jax.named_scope(f"tokwait{k}"):
            pltpu.make_async_remote_copy(
                src_ref=slot, dst_ref=slot, send_sem=t_sent.at[0], recv_sem=t_got.at[k],
                device_id={"tp": z_peer(k)}, device_id_type=MESH,
            ).wait_recv()
        tok_sibling(k, slot, slot).start()
    for k in range(n_z):
        slot = tok_rows(1 - core, (z + n_z - k) % n_z)
        with jax.named_scope(f"tokpair{k}"):
            tok_sibling(k, slot, slot).wait_recv()

    tile_m, tile_n = min(256, half), min(512, cols)
    across = cols // tile_n
    tile_s = min(64, total)
    f32 = jnp.float32

    @pl.loop(0, total // tile_s)
    def _(i):
        at = pl.ds(pl.multiple_of(i * tile_s, tile_s), tile_s)
        wide = tok[at, :].astype(f32)
        scale[at, :] = lax.rsqrt(jnp.mean(wide * wide, axis=1, keepdims=True) + 1e-06)

    def tiles(count, first, run):
        @pl.loop(0, (count // tile_m) * across)
        def _(i):
            at = pl.ds(pl.multiple_of(first + (i // across) * tile_m, tile_m), tile_m)
            run(at, pl.ds(pl.multiple_of((i % across) * tile_n, tile_n), tile_n))

    def deep(mask):
        return pl.ds(pl.multiple_of(flip_all(fs, mask, dims) * rows, rows), rows)

    def dot(x, w):
        return jnp.dot(x, w, preferred_element_type=f32)

    def piece_dot(at, to, h):
        if halves == 1:
            return dot(tok[at, deep(every)], up[deep(every), to])
        tall = part // halves
        owner = flip_all(fs, every, dims) * rows
        spots = [pl.ds(pl.multiple_of(owner + p * part + h * tall, tall), tall) for p in range(dims)]
        x = jnp.concatenate([tok[at, spot] for spot in spots], axis=1)
        return dot(x, jnp.concatenate([up[spot, to] for spot in spots], axis=0))

    for mask in range(every):
        for w in (GATE, UP):
            for p in range(dims):
                for h in range(cuts(w, mask)):
                    with jax.named_scope(f"early_need{mask}{w}{p}{h}"):
                        need(w, p, h, mask)

    def early(at, to):
        g, u = dot(tok[at, deep(0)], gate[deep(0), to]), dot(tok[at, deep(0)], up[deep(0), to])
        for mask in range(1, every):
            g = g + dot(tok[at, deep(mask)], gate[deep(mask), to])
            u = u + dot(tok[at, deep(mask)], up[deep(mask), to])
        gate_acc[at, to] = g
        up_acc[at, to] = u

    with jax.named_scope("early"):
        tiles(total, 0, early)

    for p in range(dims):
        with jax.named_scope(f"gate_need{p}"):
            need(GATE, p, 0, every)

    def gate_end(at, to):
        g = scale[at, :] * (gate_acc[at, to] + dot(tok[at, deep(every)], gate[deep(every), to]))
        gate_acc[at, to] = scale[at, :] * (g / (1.0 + jnp.exp(-g)))

    with jax.named_scope("gate_end"):
        tiles(total, 0, gate_end)

    for h in range(cuts(UP, every) - 1):
        for p in range(dims):
            with jax.named_scope(f"up_need{h}{p}"):
                need(UP, p, h, every)

        def up_more(at, to):
            up_acc[at, to] = up_acc[at, to] + piece_dot(at, to, h)

        with jax.named_scope(f"up_more{h}"):
            tiles(total, 0, up_more)

    for p in range(dims):
        with jax.named_scope(f"up_need{cuts(UP, every) - 1}{p}"):
            need(UP, p, cuts(UP, every) - 1, every)

    send_down(1, range(dims))

    def up_end(at, to):
        u = up_acc[at, to] + piece_dot(at, to, cuts(UP, every) - 1)
        hidden[at, to] = (gate_acc[at, to] * u).astype(jnp.bfloat16)

    units = [sum(tall for _, _, tall in blocks) // width for blocks, _, _ in chunks]
    bounds = [sum(units[:n]) for n in range(len(units) + 1)]
    count = len(chunks)

    def slot_rows(d):
        return pl.ds(pl.multiple_of(d * own_tok, own_tok), own_tok)

    def product(n, parity, out, slot=None):
        tile = own_tok if slot is not None else min(256, half)
        spots = []
        for mask, top, tall in chunks[n][0]:
            start = flip_all(fs, mask, dims) * rows + top
            spots.append(pl.ds(pl.multiple_of(start, math.gcd(tall, top) if top else tall), tall))

        def run(i):
            at = pl.ds(pl.multiple_of(i * tile, tile), tile)
            src = pl.ds(pl.multiple_of(parity * half + i * tile, tile), tile)
            w = [down[spot, :] for spot in spots]
            value = lax.dot_general(
                hidden[src, :], w[0] if len(w) == 1 else jnp.concatenate(w, axis=0),
                (((1,), (1,)), ((), ())), preferred_element_type=f32,
            )
            for unit in range(units[n]):
                out(unit)[at, :] = value[:, unit * width:(unit + 1) * width].astype(out(unit).dtype)

        if slot is not None:
            run(slot)
        else:
            pl.loop(0, half // tile)(run)

    def pair_copy(n, i=None, slot=None):
        mine = pl.ds(bounds[n], units[n])
        at = (mine,) if slot is None else (mine, slot_rows(slot))
        return pltpu.make_async_remote_copy(
            src_ref=pair_send.at[at], dst_ref=pair_recv.at[at],
            send_sem=p_sent.at[0], recv_sem=p_got.at[n if i is None else count + i],
            device_id={"tp": sibling}, device_id_type=MESH,
        )

    def passing(side, hops):
        return hops - 1 if side > 0 else n_z - 1 - hops

    deal = units[0]
    meets = range(first, count - 1 if n_z > 3 else first)

    def chain_copy(n, side, hops):
        mine = pl.ds(n * deal, deal)
        if hops == 1:
            dst, got = z_last.at[(1 - side) // 2, mine], l_got.at[(1 - side) // 2]
        else:
            dst, got = z_pass.at[mine, passing(side, hops - 1)], z_got.at[n, passing(side, hops - 1)]
        to = jnp.clip(z + side, 0, n_z - 1)
        return pltpu.make_async_remote_copy(
            src_ref=z_send.at[mine, slot_rows(jnp.clip(z + side * hops, 0, n_z - 1)), :], dst_ref=dst,
            send_sem=z_sent.at[0], recv_sem=got,
            device_id={"tp": to * 2 + core}, device_id_type=MESH,
        )

    def straight_copy(n, k):
        mine = pl.ds(bounds[n], units[n])
        return pltpu.make_async_remote_copy(
            src_ref=z_send.at[mine, slot_rows((z + k) % n_z), :], dst_ref=z_pass.at[mine, k - 1],
            send_sem=z_sent.at[0], recv_sem=z_got.at[n, k - 1],
            device_id={"tp": z_peer(k)}, device_id_type=MESH,
        )

    def meet_copy(n, to):
        mine = pl.ds(bounds[n], units[n])
        return pltpu.make_async_remote_copy(
            src_ref=z_send.at[mine, slot_rows(to), :], dst_ref=z_last.at[0, mine],
            send_sem=z_sent.at[0], recv_sem=m_got.at[n - first],
            device_id={"tp": jnp.where(z == 0, 1, n_z - 2) * 2 + core}, device_id_type=MESH,
        )

    def meet(n):
        for at, to in ((1, n_z - 1), (n_z - 2, 0)):
            @pl.when(z == at)
            def _():
                meet_copy(n, to).wait_recv()
                for unit in range(bounds[n], bounds[n + 1]):
                    rest = slice(to * own_tok, (to + 1) * own_tok)
                    both = z_send[unit, rest, :].astype(f32) + z_last[0, unit].astype(f32)
                    z_send[unit, rest, :] = both.astype(jnp.bfloat16)
                straight_copy(n, (to - at) % n_z).start()

    def at_ends(run):
        for side, end in ((1, 0), (-1, n_z - 1)):
            @pl.when(z == end)
            def _():
                run(side)

    def finish(n):
        pair_copy(n).wait_recv()
        for unit in range(units[n]):
            at = bounds[n] + unit
            z_send[at] = (pair_own[n % 2, unit] + pair_recv[at].astype(f32)).astype(jnp.bfloat16)
        if n in meets:
            for k in range(n_z - 1, 0, -1):
                hop = jnp.where(z < n_z // 2, k, n_z - k)
                to = (z + hop) % n_z
                across_all = ((z == 0) & (to == n_z - 1)) | ((z == n_z - 1) & (to == 0))
                waits = ((z == 1) & (to == n_z - 1)) | ((z == n_z - 2) & (to == 0))

                @pl.when(across_all)
                def _():
                    meet_copy(n, to).start()

                @pl.when(jnp.logical_not(across_all | waits))
                def _():
                    straight_copy(n, hop).start()
        elif n >= first:
            for k in range(n_z - 1, 0, -1):
                straight_copy(n, jnp.where(z < n_z // 2, k, n_z - k)).start()
        else:
            at_ends(lambda side: [chain_copy(n, side, hops).start() for hops in range(n_z - 1, 0, -1)])

    def pass_on(n, depth, side):
        mine = pl.ds(n * deal, deal)
        for hops in range(n_z - 2, 0, -1):
            @pl.when(depth + hops < n_z)
            def _():
                at = passing(side, hops)
                pltpu.make_async_remote_copy(
                    src_ref=z_pass.at[mine, at], dst_ref=z_pass.at[mine, at],
                    send_sem=z_sent.at[0], recv_sem=z_got.at[n, at],
                    device_id={"tp": sibling}, device_id_type=MESH,
                ).wait_recv()
                to = slot_rows(jnp.clip(z + side * hops, 0, n_z - 1))
                both = z_send[mine, to, :].astype(f32) + z_pass[mine, at].astype(f32)
                z_send[mine, to, :] = both.astype(jnp.bfloat16)
                chain_copy(n, side, hops).start()

    def relay(t):
        for side in (1, -1):
            depth = z if side > 0 else n_z - 1 - z
            inner = (depth > 0) & (depth < n_z - 1)
            for late in (1, 0):
                n = t - depth - late
                slow = (n < 2) | ((n == first - 1) & (depth > 1))
                turn = inner & (n >= 0) & (n < first) & (slow if late else jnp.logical_not(slow))

                @pl.when(turn)
                def _():
                    pass_on(n, depth, side)

    def open_up():
        slots = [jnp.where(z < n_z // 2, n_z - 1 - i, i) for i in range(n_z)]

        def half_of(parity, slot):
            first_row = parity * half + slot * own_tok
            at = pl.ds(pl.multiple_of(first_row, own_tok), own_tok)
            for j in range(across):
                up_end(at, slice(j * tile_n, (j + 1) * tile_n))

        def away(i):
            half_of(1 - core, slots[i])
            product(0, 1 - core, lambda unit: pair_send.at[unit], slots[i])
            pair_copy(0, i, slots[i]).start()

        def close(i):
            half_of(core, slots[i])
            product(0, core, lambda unit: pair_own.at[0, unit], slots[i])
            pair_copy(0, i, slots[i]).wait_recv()
            here = slot_rows(slots[i])
            for unit in range(deal):
                own = pair_own[0, unit, here, :] + pair_recv[unit, here, :].astype(f32)
                z_send[unit, here, :] = own.astype(jnp.bfloat16)
            if i < n_z - 1:
                at_ends(lambda side: chain_copy(0, side, n_z - 1 - i).start())

        for i in range(n_z):
            with jax.named_scope(f"away{i}"):
                away(i)
            if i:
                with jax.named_scope(f"close{i - 1}"):
                    close(i - 1)
        with jax.named_scope(f"close{n_z - 1}"):
            close(n_z - 1)

    with jax.named_scope("open"):
        open_up()
    finished = 1
    for n, (blocks, needs, wave) in enumerate(chunks):
        if n == 0:
            continue
        if split and n == 3:
            send_down(0, range(1, dims))
        for p, h, mask in needs:
            with jax.named_scope(f"d{n}_need"):
                need(DOWN, p, h, mask, hold=split and n in (2, 3))
        if split and n == 3:
            for p, h, mask in chunks[2][1] + chunks[3][1]:
                forward(DOWN, p, h, mask)
        with jax.named_scope(f"d{n}_prodA"):
            product(n, 1 - core, lambda unit: pair_send.at[bounds[n] + unit])
            pair_copy(n).start()
        if n >= first:
            with jax.named_scope(f"d{n}_relay"):
                relay(n)
                if n - 2 in meets:
                    meet(n - 2)
        with jax.named_scope(f"d{n}_finish"):
            if finished < n:
                finish(n - 1)
                finished = n
        with jax.named_scope(f"d{n}_prodB"):
            product(n, core, lambda unit: pair_own.at[n % 2, unit])
        if n + 1 == count or chunks[n + 1][2] != wave:
            with jax.named_scope(f"d{n}_finish"):
                finish(n)
                finished = n + 1
        if n < first:
            with jax.named_scope(f"d{n}_relay"):
                relay(n)
    with jax.named_scope("lastrelay"):
        for t in range(count, first + n_z):
            relay(t)
        for n in meets:
            if n + 2 >= count:
                meet(n)

    mine = slot_rows(z)

    def total_of(unit):
        branch = z_send[unit, mine, :].astype(f32)
        if unit < bounds[first]:
            return branch + z_last[0, unit].astype(f32) + z_last[1, unit].astype(f32)
        for k in range(n_z - 1):
            branch = branch + z_pass[unit, k].astype(f32)
        return branch

    def settle(mask, top, parts):
        start = flip_all(fs, mask, dims) * rows + top
        to = pl.ds(pl.multiple_of(start, width), width)
        branch = jnp.concatenate(parts, axis=1) if len(parts) > 1 else parts[0]
        mixed[:, to] = (tok_in[:, to].astype(f32) + 0.5 * branch).astype(jnp.bfloat16)

    with jax.named_scope("lastwait"):
        spread = pl.ds(0, bounds[first])
        for side, end in ((0, 0), (1, n_z - 1)):
            @pl.when(z != end)
            def _():
                pltpu.make_async_remote_copy(
                    src_ref=z_last.at[side, spread], dst_ref=z_last.at[side, spread],
                    send_sem=z_sent.at[0], recv_sem=l_got.at[side],
                    device_id={"tp": sibling}, device_id_type=MESH,
                ).wait_recv()
    open_parts = {}
    for n, (blocks, _, _) in enumerate(chunks):
        with jax.named_scope(f"last{n}"):
            if n >= first:
                for k in range(1, n_z):
                    absent = ((z == n_z - 1) & (k == n_z - 1)) | ((z == 0) & (k == 1))
                    if n not in meets:
                        straight_copy(n, k).wait_recv()
                    elif k in (1, n_z - 1):
                        @pl.when(jnp.logical_not(absent))
                        def _():
                            straight_copy(n, k).wait_recv()

                        @pl.when(absent)
                        def _():
                            spread = pl.ds(bounds[n], units[n])
                            z_pass[spread, k - 1] = jnp.zeros((units[n], own_tok, width), jnp.bfloat16)
                    else:
                        straight_copy(n, k).wait_recv()
            sums = [total_of(unit) for unit in range(bounds[n], bounds[n + 1])]
            lane = 0
            for mask, top, tall in blocks:
                if tall < width:
                    key = (mask, top // width * width)
                    open_parts.setdefault(key, []).append(sums[0][:, lane:lane + tall])
                    lane += tall
                    if sum(piece.shape[1] for piece in open_parts[key]) == width:
                        settle(mask, key[1], open_parts.pop(key))
                    continue
                for at in range(0, tall, width):
                    settle(mask, top + at, [sums[lane // width]])
                    lane += width

    def sent(ref, sem):
        pltpu.make_async_remote_copy(
            src_ref=ref, dst_ref=ref, send_sem=sem, recv_sem=sem,
            device_id={"tp": sibling}, device_id_type=MESH,
        ).wait_send()

    for w in range(3):
        sent(ready[w].at[pl.ds(0, every * rows), :], w_sent.at[w])
    sent(tok.at[pl.ds(0, (2 * n_z - 1) * own_tok), :], t_sent.at[0])
    sent(pair_send, p_sent.at[0])
    sent(z_pass, z_sent.at[0])


def store(*refs):
    count = len(refs) // 2
    done = refs[-1]
    copies = []
    for n in range(count):
        tall = refs[n].shape[0] // 2
        for h in range(2):
            at = pl.ds(h * tall, tall)
            copies.append(pltpu.make_async_copy(refs[n].at[at, :], refs[count + n].at[at, :], done.at[n, h]))
            copies[-1].start()
    for copy in copies:
        copy.wait()


def body(n_fs, n_tp, tokens, norm_gain, gate_master, up_master, down_master):
    own_tok, depth = tokens.shape
    rows, cols = gate_master.shape
    dims = n_fs.bit_length() - 1
    n_z = n_tp // 2
    half, total = n_z * own_tok, n_tp * own_tok
    part = rows // dims
    halves = part // 128 if part % 128 == 0 else 1
    late_tall, tall_of, width, chunks, first = plan(n_fs, dims, rows)
    count, deal = n_fs * rows // width, sum(tall for _, _, tall in chunks[0][0]) // width
    steps = len(chunks)
    pieces = dims * ((n_fs - 1) * (1 + halves) + (n_fs - 2) * (part // tall_of) + part // late_tall)
    bf16, f32 = jnp.bfloat16, jnp.float32
    dma = pltpu.SemaphoreType.DMA
    vmem = pl.BlockSpec(memory_space=pltpu.VMEM)
    hbm = pl.BlockSpec(memory_space=pltpu.HBM)
    operands = (tokens, norm_gain[None, :], gate_master, up_master, down_master)
    results = pl.pallas_call(
        functools.partial(kernel, n_fs, n_z, dims, halves, late_tall, tall_of, width, chunks, first),
        out_shape=(pltpu.VMEM((own_tok, depth), bf16),)
        + tuple(pltpu.VMEM((n_fs * rows, cols), bf16) for _ in range(3)),
        in_specs=[hbm] * 5,
        out_specs=(vmem,) * 4,
        scratch_shapes=[
            pltpu.VMEM((own_tok, depth), bf16),
            pltpu.VMEM((1, rows), f32),
            pltpu.VMEM((rows, 128), f32),
            pltpu.VMEM((3, rows, cols), f32),
            pltpu.VMEM((total, depth), bf16),
            pltpu.VMEM((total, 1), f32),
            pltpu.VMEM((total, cols), f32),
            pltpu.VMEM((total, cols), f32),
            pltpu.VMEM((total, cols), bf16),
            pltpu.VMEM((2, deal, half, width), f32),
            pltpu.VMEM((count, half, width), bf16),
            pltpu.VMEM((count, half, width), bf16),
            pltpu.VMEM((count, half, width), bf16),
            pltpu.VMEM((count, n_z - 1, own_tok, width), bf16),
            pltpu.VMEM((2, count, own_tok, width), bf16),
            dma((3,)), dma((pieces,)),
            dma((1,)), dma((n_z,)), dma((n_z,)),
            dma((1,)), dma((steps + n_z,)),
            dma((1,)), dma((steps, n_z - 1)), dma((2,)), dma((steps - first,)),
            dma((4 * dims + 3,)),
        ],
        compiler_params=pltpu.CompilerParams(
            collective_id=0, has_side_effects=True, vmem_limit_bytes=40 * 1024 * 1024
        ),
    )(*(pltpu.with_memory_space_constraint(value, pltpu.HBM) for value in operands))
    return pl.pallas_call(
        store,
        out_shape=tuple(jax.ShapeDtypeStruct(result.shape, result.dtype) for result in results),
        in_specs=[vmem] * 4,
        out_specs=(hbm,) * 4,
        scratch_shapes=[dma((4, 2))],
        compiler_params=pltpu.CompilerParams(vmem_limit_bytes=1024 * 1024),
    )(*(pltpu.with_memory_space_constraint(result, pltpu.VMEM) for result in results))


def solution(mesh):
    in_specs = (P(("fs", "tp"), None), P("fs"), P("fs", "tp"), P("fs", "tp"), P("fs", "tp"))
    out_specs = (P(("fs", "tp"), None), P(None, "tp"), P(None, "tp"), P(None, "tp"))
    step = functools.partial(body, mesh.shape["fs"], mesh.shape["tp"])
    return jax.shard_map(step, mesh=mesh, in_specs=in_specs, out_specs=out_specs, check_vma=False)
```

```python
import functools
import math

import jax
import jax.numpy as jnp
from jax import lax
from jax.experimental import pallas as pl
from jax.experimental.pallas import tpu as pltpu
from jax.sharding import PartitionSpec as P

MESH = pl.DeviceIdType.MESH
GATE, UP, DOWN = 0, 1, 2


def flip(index, bit):
    return index + bit - 2 * bit * ((index // bit) % 2)


def flip_all(index, mask, dims):
    for dim in range(dims):
        if mask >> dim & 1:
            index = flip(index, 1 << dim)
    return index


def span(bits):
    masks = [0]
    for bit in bits:
        masks += [mask | bit for mask in masks]
    return masks


def plan(n_fs, dims, rows):
    part = rows // dims
    last = n_fs - 1
    if dims != 2 or part % 128 or rows % 256:
        chunks = [([(mask, 0, rows)], [(p, 0, mask) for p in range(dims)], mask) for mask in range(n_fs)]
        return [part], [part], rows, chunks, last
    late, other = [64] * (part // 64), [128] * (part // 128)
    chunks = [([(0, at, 256)], [], 0) for at in range(0, rows, 256)]
    for step, owners in enumerate(([(1, 0), (2, 1)], [(2, 0), (1, 1)], [(last, 0), (last, 1)])):
        heights = late if step == 2 else other
        for h, tall in enumerate(heights):
            blocks = [(mask, p * part + sum(heights[:h]), tall) for mask, p in owners]
            chunks.append((blocks, [(p, h, mask) for mask, p in owners], (step, h)))
    return late, other, 128, chunks, next(n for n, chunk in enumerate(chunks) if chunk[2] == (1, len(other) - 1))


def kernel(
    n_fs, n_z, dims, halves, late, other, width, chunks, first,
    tok_hbm, gain_hbm, gate_hbm, up_hbm, down_hbm,
    mixed, gate, up, down,
    tok_in, gain_row, gain, masters, tok, scale, gate_acc, up_acc, hidden, pair_own, pair_send, pair_recv, z_send, z_pass, z_last,
    w_sent, w_got, t_sent, t_got, s_got, p_sent, p_got, z_sent, z_got, l_got, f_got, m_got, loaded,
):
    fs, tp = lax.axis_index("fs"), lax.axis_index("tp")
    z, core = tp // 2, tp % 2
    sibling = z * 2 + 1 - core
    rows, cols = gate_hbm.shape
    part = rows // dims
    own_tok = tok_in.shape[0]
    half = n_z * own_tok
    total = 2 * half
    ready = (gate, up, down)
    every = n_fs - 1

    def heights(w, mask):
        if w == DOWN:
            return late if mask == every else other
        many = (1, halves)[w]
        return [part // many] * many

    def cuts(w, mask):
        return len(heights(w, mask))

    loads = {}
    reads = [("gain", gain_hbm, gain_row)]
    for w, master in ((GATE, gate_hbm), (UP, up_hbm)):
        for p in range(dims):
            for i in range(2):
                mine = pl.ds(p * part + i * part // 2, part // 2)
                reads.append(((w, p, i), master.at[mine, :], masters.at[w, mine, :]))
    reads.append(("tok", tok_hbm, tok_in))
    reads.append(("down", down_hbm, masters.at[DOWN]))
    for n, (name, src, dst) in enumerate(reads):
        loads[name] = pltpu.make_async_copy(src, dst, loaded.at[n])

    def z_peer(k):
        return ((z + k) % n_z) * 2 + core

    for name, _, _ in reads[:1 + 2 * dims]:
        loads[name].start()
    barrier = pltpu.get_barrier_semaphore()
    for dim in range(dims):
        pl.semaphore_signal(barrier, 1, device_id={"fs": flip(fs, 1 << dim)}, device_id_type=MESH)
    for k in range(1, n_z):
        pl.semaphore_signal(barrier, 1, device_id={"tp": z_peer(k)}, device_id_type=MESH)
    pl.semaphore_signal(barrier, 1, device_id={"tp": sibling}, device_id_type=MESH)

    loads["gain"].wait()
    for n in range(rows // 128):
        line = gain_row[:, n * 128:(n + 1) * 128]
        gain[n * 128:(n + 1) * 128, :] = jnp.transpose(jnp.broadcast_to(line, (128, 128)))

    def block(w, owner, p, h, mask):
        tall, top = heights(w, mask)[h], sum(heights(w, mask)[:h])
        start = flip_all(fs, owner, dims) * rows + p * part + top
        return ready[w].at[pl.ds(pl.multiple_of(start, tall), tall), :]

    def order(p):
        return [1 << ((p + s) % dims) for s in range(dims)]

    arrivals = {
        (p, held | order(p)[stage]): stage
        for p in range(dims) for stage in range(dims) for held in span(order(p)[:stage])
    }
    arrived = set()

    def together(w, p, h, mask):
        if dims != 2:
            return [(p, mask)]
        return sorted([(p, mask), (1 - p, mask if mask == every else every - mask)])

    place = {}
    for w in (GATE, UP, DOWN):
        for p in range(dims):
            for mask in range(1, n_fs):
                for h in range(cuts(w, mask)):
                    place.setdefault((w, h, *together(w, p, h, mask)), len(place))

    def got(w, p, h, mask):
        return w_got.at[place[(w, h, *together(w, p, h, mask))]]

    def weight_copy(w, p, h, held, mask, stage):
        return pltpu.make_async_remote_copy(
            src_ref=block(w, held, p, h, mask), dst_ref=block(w, held, p, h, mask),
            send_sem=w_sent.at[w], recv_sem=got(w, p, h, mask),
            device_id={"fs": flip(fs, order(p)[stage])}, device_id_type=MESH,
        )

    def send(w, p, h, stage, held):
        weight_copy(w, p, h, held, held | order(p)[stage], stage).start()

    def need(w, p, h, mask, hold=False):
        if mask and (w, p, h, mask) not in arrived:
            pair = together(w, p, h, mask)
            tall = heights(w, mask)[h] * len(pair)
            here = ready[w].at[pl.ds(0, tall), :] if len(pair) > 1 else block(w, mask, p, h, mask)
            pltpu.make_async_remote_copy(
                src_ref=here, dst_ref=here, send_sem=w_sent.at[w], recv_sem=got(w, p, h, mask),
                device_id={"fs": flip(fs, 1)}, device_id_type=MESH,
            ).wait_recv()
            for p, mask in pair:
                arrived.add((w, p, h, mask))
                if not hold:
                    forward(w, p, h, mask)

    def forward(w, p, h, mask):
        for later in range(arrivals[p, mask] + 1, dims):
            top, finer = sum(heights(w, mask)[:h]), heights(w, mask | order(p)[later])
            for piece in range(len(finer)):
                if top <= sum(finer[:piece]) < top + heights(w, mask)[h]:
                    send(w, p, piece, later, mask)

    def relays(ws):
        for stage in range(dims - 1):
            for w in ws:
                for p in range(dims):
                    for held in span(order(p)[:stage]):
                        for h in range(cuts(w, held | order(p)[stage])):
                            need(w, p, h, held | order(p)[stage])

    def prepare(w, top, tall):
        mine = slice(top, top + tall)
        value = masters[w, mine, :]
        if w != DOWN:
            value = gain[mine, 0:1] * value
        ready[w][pl.ds(pl.multiple_of(fs * rows + top, tall), tall), :] = value.astype(jnp.bfloat16)

    short = part // 2
    for p in range(dims):
        for i in range(2):
            loads[GATE, p, i].wait()
            prepare(GATE, p * part + i * short, short)
            if p == 0 and i == 0:
                with jax.named_scope("barrier"):
                    pl.semaphore_wait(barrier, dims + n_z)
            at = gate.at[pl.ds(pl.multiple_of(fs * rows + p * part + i * short, short), short), :]
            pltpu.make_async_remote_copy(
                src_ref=at, dst_ref=at, send_sem=w_sent.at[GATE], recv_sem=got(GATE, p, 0, order(p)[0]),
                device_id={"fs": flip(fs, order(p)[0])}, device_id_type=MESH,
            ).start()
    for name, _, _ in reads[1 + 2 * dims:]:
        loads[name].start()
    for p in range(dims):
        for i in range(2):
            loads[UP, p, i].wait()
        prepare(UP, p * part, part)
        for h in range(cuts(UP, 0)):
            send(UP, p, h, 0, 0)

    def tok_rows(c, chip):
        start = (c * n_z + chip) * own_tok
        return tok.at[pl.ds(pl.multiple_of(start, own_tok), own_tok), :]

    def tok_z(k):
        return pltpu.make_async_remote_copy(
            src_ref=tok_in, dst_ref=tok_rows(core, z), send_sem=t_sent.at[0], recv_sem=t_got.at[k - 1],
            device_id={"tp": z_peer(k)}, device_id_type=MESH,
        )

    def tok_sibling(src, slot):
        return pltpu.make_async_remote_copy(
            src_ref=src, dst_ref=slot, send_sem=t_sent.at[0], recv_sem=s_got.at[0],
            device_id={"tp": sibling}, device_id_type=MESH,
        )

    loads["tok"].wait()
    for k in range(1, n_z):
        tok_z(k).start()
    tok_sibling(tok_in, tok_rows(core, z)).start()
    for w in (GATE, UP):
        for p in range(dims):
            for stage in range(1, dims):
                for h in range(cuts(w, 0)):
                    send(w, p, h, stage, 0)
    tok_rows(core, z)[...] = tok_in[...]
    loads["down"].wait()
    for p in range(dims):
        prepare(DOWN, p * part, part)

    @pl.when(z == 0)
    def _():
        z_last[0] = jnp.zeros(z_last.shape[1:], jnp.bfloat16)

    @pl.when(z == n_z - 1)
    def _():
        z_last[1] = jnp.zeros(z_last.shape[1:], jnp.bfloat16)

    with jax.named_scope("relays"):
        relays((GATE, UP))

    def send_down(turn, stages):
        @pl.when(core == turn)
        def _():
            for stage in stages:
                for h in range(max(cuts(DOWN, order(p)[stage]) for p in range(dims))):
                    for p in range(dims):
                        send(DOWN, p, h, stage, 0)

    split = dims == 2 and first > 4
    send_down(0, range(1) if split else range(dims))

    for k in range(1, n_z):
        slot = tok_rows(core, (z + n_z - k) % n_z)
        with jax.named_scope(f"tokwait{k}"):
            pltpu.make_async_remote_copy(
                src_ref=slot, dst_ref=slot, send_sem=t_sent.at[0], recv_sem=t_got.at[k - 1],
                device_id={"tp": z_peer(k)}, device_id_type=MESH,
            ).wait_recv()
        tok_sibling(slot, slot).start()
    rest = tok.at[pl.ds(pl.multiple_of((1 - core) * half, half), half), :]
    with jax.named_scope("tokpair"):
        pltpu.make_async_remote_copy(
            src_ref=rest, dst_ref=rest, send_sem=t_sent.at[0], recv_sem=s_got.at[0],
            device_id={"tp": sibling}, device_id_type=MESH,
        ).wait_recv()

    tile_m, tile_n = min(256, half), min(512, cols)
    across = cols // tile_n
    tile_s = min(64, total)
    f32 = jnp.float32

    @pl.loop(0, total // tile_s)
    def _(i):
        at = pl.ds(pl.multiple_of(i * tile_s, tile_s), tile_s)
        wide = tok[at, :].astype(f32)
        scale[at, :] = lax.rsqrt(jnp.mean(wide * wide, axis=1, keepdims=True) + 1e-06)

    def tiles(count, first, run):
        @pl.loop(0, (count // tile_m) * across)
        def _(i):
            at = pl.ds(pl.multiple_of(first + (i // across) * tile_m, tile_m), tile_m)
            run(at, pl.ds(pl.multiple_of((i % across) * tile_n, tile_n), tile_n))

    def deep(mask):
        return pl.ds(pl.multiple_of(flip_all(fs, mask, dims) * rows, rows), rows)

    def dot(x, w):
        return jnp.dot(x, w, preferred_element_type=f32)

    def piece_dot(at, to, h):
        if halves == 1:
            return dot(tok[at, deep(every)], up[deep(every), to])
        tall = part // halves
        owner = flip_all(fs, every, dims) * rows
        spots = [pl.ds(pl.multiple_of(owner + p * part + h * tall, tall), tall) for p in range(dims)]
        x = jnp.concatenate([tok[at, spot] for spot in spots], axis=1)
        return dot(x, jnp.concatenate([up[spot, to] for spot in spots], axis=0))

    for mask in range(every):
        for w in (GATE, UP):
            for p in range(dims):
                for h in range(cuts(w, mask)):
                    with jax.named_scope(f"early_need{mask}{w}{p}{h}"):
                        need(w, p, h, mask)

    def early(at, to):
        g, u = dot(tok[at, deep(0)], gate[deep(0), to]), dot(tok[at, deep(0)], up[deep(0), to])
        for mask in range(1, every):
            g = g + dot(tok[at, deep(mask)], gate[deep(mask), to])
            u = u + dot(tok[at, deep(mask)], up[deep(mask), to])
        gate_acc[at, to] = g
        up_acc[at, to] = u

    with jax.named_scope("early"):
        tiles(total, 0, early)

    for p in range(dims):
        with jax.named_scope(f"gate_need{p}"):
            need(GATE, p, 0, every)

    def gate_end(at, to):
        g = scale[at, :] * (gate_acc[at, to] + dot(tok[at, deep(every)], gate[deep(every), to]))
        gate_acc[at, to] = scale[at, :] * (g / (1.0 + jnp.exp(-g)))

    with jax.named_scope("gate_end"):
        tiles(total, 0, gate_end)

    for h in range(cuts(UP, every) - 1):
        for p in range(dims):
            with jax.named_scope(f"up_need{h}{p}"):
                need(UP, p, h, every)

        def up_more(at, to):
            up_acc[at, to] = up_acc[at, to] + piece_dot(at, to, h)

        with jax.named_scope(f"up_more{h}"):
            tiles(total, 0, up_more)

    for p in range(dims):
        with jax.named_scope(f"up_need{cuts(UP, every) - 1}{p}"):
            need(UP, p, cuts(UP, every) - 1, every)

    send_down(1, range(dims))

    def up_end(at, to):
        u = up_acc[at, to] + piece_dot(at, to, cuts(UP, every) - 1)
        hidden[at, to] = (gate_acc[at, to] * u).astype(jnp.bfloat16)

    spans = [sum(tall for _, _, tall in blocks) for blocks, _, _ in chunks]
    units = [max(1, wide // width) for wide in spans]
    narrow = [wide < width for wide in spans]
    bounds = [sum(units[:n]) for n in range(len(units) + 1)]
    count = len(chunks)

    def slot_rows(d):
        return pl.ds(pl.multiple_of(d * own_tok, own_tok), own_tok)

    def product(n, parity, out, slot=None):
        tile = own_tok if slot is not None else min(256, half)
        spots = []
        for mask, top, tall in chunks[n][0]:
            start = flip_all(fs, mask, dims) * rows + top
            spots.append(pl.ds(pl.multiple_of(start, math.gcd(tall, top) if top else tall), tall))

        def run(i):
            at = pl.ds(pl.multiple_of(i * tile, tile), tile)
            src = pl.ds(pl.multiple_of(parity * half + i * tile, tile), tile)
            w = [down[spot, :] for spot in spots]
            value = lax.dot_general(
                hidden[src, :], w[0] if len(w) == 1 else jnp.concatenate(w, axis=0),
                (((1,), (1,)), ((), ())), preferred_element_type=f32,
            )
            if narrow[n]:
                value = jnp.concatenate([
                    jnp.concatenate([value[r:r + own_tok // 2], value[r + own_tok // 2:r + own_tok]], axis=1)
                    for r in range(0, tile, own_tok)
                ], axis=0)
                at = pl.ds(pl.multiple_of(i * (tile // 2), tile // 2), tile // 2)
            for unit in range(units[n]):
                out(unit)[at, :] = value[:, unit * width:(unit + 1) * width].astype(out(unit).dtype)

        if slot is not None:
            run(slot)
        else:
            pl.loop(0, half // tile)(run)

    def pair_copy(n, i=None, slot=None):
        mine = pl.ds(bounds[n], units[n])
        at = (mine, pl.ds(0, half // 2 if narrow[n] else half)) if slot is None else (mine, slot_rows(slot))
        return pltpu.make_async_remote_copy(
            src_ref=pair_send.at[at], dst_ref=pair_recv.at[at],
            send_sem=p_sent.at[0], recv_sem=p_got.at[n if i is None else count + i],
            device_id={"tp": sibling}, device_id_type=MESH,
        )

    def passing(side, hops):
        return hops - 1 if side > 0 else n_z - 1 - hops

    deal = units[0]
    meets = range(first, count - 1 if n_z > 3 else first)
    low_meets = range(first, max(first, meets.stop - 1))
    lasting = range(max(first, count - 2), count)

    def chain_copy(n, side, hops):
        mine = pl.ds(n * deal, deal)
        if hops == 1:
            dst, got = z_last.at[(1 - side) // 2, mine], l_got.at[(1 - side) // 2]
        else:
            dst, got = z_pass.at[mine, passing(side, hops - 1)], z_got.at[n, passing(side, hops - 1)]
        to = jnp.clip(z + side, 0, n_z - 1)
        return pltpu.make_async_remote_copy(
            src_ref=z_send.at[mine, slot_rows(jnp.clip(z + side * hops, 0, n_z - 1)), :], dst_ref=dst,
            send_sem=z_sent.at[0], recv_sem=got,
            device_id={"tp": to * 2 + core}, device_id_type=MESH,
        )

    def straight_copy(n, k):
        mine = pl.ds(bounds[n], units[n])
        tall = own_tok // 2 if narrow[n] else own_tok
        at = pl.ds(pl.multiple_of(((z + k) % n_z) * tall, tall), tall)
        return pltpu.make_async_remote_copy(
            src_ref=z_send.at[mine, at, :], dst_ref=z_pass.at[mine, k - 1, pl.ds(0, tall)],
            send_sem=z_sent.at[0], recv_sem=f_got.at[n - first],
            device_id={"tp": z_peer(k)}, device_id_type=MESH,
        )

    def meet_copy(n, to):
        mine = pl.ds(bounds[n], units[n])
        return pltpu.make_async_remote_copy(
            src_ref=z_send.at[mine, slot_rows(to), :], dst_ref=z_last.at[0, mine],
            send_sem=z_sent.at[0], recv_sem=m_got.at[n - first],
            device_id={"tp": jnp.where(z == 0, 1, n_z - 2) * 2 + core}, device_id_type=MESH,
        )

    def meet(n):
        for at, to in ((1, n_z - 1), (n_z - 2, 0))[:2 if n in low_meets else 1]:
            @pl.when(z == at)
            def _():
                meet_copy(n, to).wait_recv()
                for unit in range(bounds[n], bounds[n + 1]):
                    rest = slice(to * own_tok, (to + 1) * own_tok)
                    both = z_send[unit, rest, :].astype(f32) + z_last[0, unit].astype(f32)
                    z_send[unit, rest, :] = both.astype(jnp.bfloat16)
                straight_copy(n, (to - at) % n_z).start()

    def held(n, to):
        inner = (z > 0) & (z < n_z - 1)
        low = (to > 0) & (to < z) if n in lasting else to < 0
        return low | (inner & (to == z + 1)) if n == count - 1 else low

    def at_ends(run):
        for side, end in ((1, 0), (-1, n_z - 1)):
            @pl.when(z == end)
            def _():
                run(side)

    def finish(n):
        pair_copy(n).wait_recv()
        for unit in range(units[n]):
            at, rest = bounds[n] + unit, slice(0, half // 2 if narrow[n] else half)
            z_send[at, rest, :] = (pair_own[n % 2, unit, rest, :] + pair_recv[at, rest, :].astype(f32)).astype(jnp.bfloat16)
        if n >= first:
            for k in range(n_z - 1, 0, -1):
                hop = jnp.where(z < n_z // 2, k, n_z - k)
                to = (z + hop) % n_z
                later = held(n, to)
                if n in meets:
                    over, waits = (z == 0) & (to == n_z - 1), (z == 1) & (to == n_z - 1)
                    if n in low_meets:
                        over, waits = over | ((z == n_z - 1) & (to == 0)), waits | ((z == n_z - 2) & (to == 0))

                    @pl.when(over)
                    def _():
                        meet_copy(n, to).start()

                    later = later | over | waits

                @pl.when(jnp.logical_not(later))
                def _():
                    straight_copy(n, hop).start()
        else:
            at_ends(lambda side: [chain_copy(n, side, hops).start() for hops in range(n_z - 1, 0, -1)])

    def pass_on(n, depth, side):
        mine = pl.ds(n * deal, deal)
        for hops in range(n_z - 2, 0, -1):
            @pl.when(depth + hops < n_z)
            def _():
                at = passing(side, hops)
                pltpu.make_async_remote_copy(
                    src_ref=z_pass.at[mine, at], dst_ref=z_pass.at[mine, at],
                    send_sem=z_sent.at[0], recv_sem=z_got.at[n, at],
                    device_id={"tp": sibling}, device_id_type=MESH,
                ).wait_recv()
                to = slot_rows(jnp.clip(z + side * hops, 0, n_z - 1))
                both = z_send[mine, to, :].astype(f32) + z_pass[mine, at].astype(f32)
                z_send[mine, to, :] = both.astype(jnp.bfloat16)
                chain_copy(n, side, hops).start()

    def relay(t):
        for side in (1, -1):
            depth = z if side > 0 else n_z - 1 - z
            inner = (depth > 0) & (depth < n_z - 1)
            for later in (1, 0):
                n = t - depth - later
                far = (depth > 1) * 1
                lag = (n < 2) * 1 + (n == first - 1) * far
                turn = inner & (n >= 0) & (n < first) & (lag == later)

                @pl.when(turn)
                def _():
                    pass_on(n, depth, side)

    def open_up():
        slots = [jnp.where(z < n_z // 2, n_z - 1 - i, i) for i in range(n_z)]

        def half_of(parity, slot):
            first_row = parity * half + slot * own_tok
            at = pl.ds(pl.multiple_of(first_row, own_tok), own_tok)
            for j in range(across):
                up_end(at, slice(j * tile_n, (j + 1) * tile_n))

        def away(i):
            half_of(1 - core, slots[i])
            product(0, 1 - core, lambda unit: pair_send.at[unit], slots[i])
            pair_copy(0, i, slots[i]).start()

        def close(i):
            half_of(core, slots[i])
            product(0, core, lambda unit: pair_own.at[0, unit], slots[i])
            pair_copy(0, i, slots[i]).wait_recv()
            here = slot_rows(slots[i])
            for unit in range(deal):
                own = pair_own[0, unit, here, :] + pair_recv[unit, here, :].astype(f32)
                z_send[unit, here, :] = own.astype(jnp.bfloat16)
            if i < n_z - 1:
                at_ends(lambda side: chain_copy(0, side, n_z - 1 - i).start())

        for i in range(n_z):
            with jax.named_scope(f"away{i}"):
                away(i)
            if i:
                with jax.named_scope(f"close{i - 1}"):
                    close(i - 1)
        with jax.named_scope(f"close{n_z - 1}"):
            close(n_z - 1)

    with jax.named_scope("open"):
        open_up()
    finished = 1
    for n, (blocks, needs, wave) in enumerate(chunks):
        if n == 0:
            continue
        if split and n == 3:
            send_down(0, range(1, dims))
        for p, h, mask in needs:
            with jax.named_scope(f"d{n}_need"):
                need(DOWN, p, h, mask, hold=split and n in (2, 3))
        if split and n == 3:
            for p, h, mask in chunks[2][1] + chunks[3][1]:
                forward(DOWN, p, h, mask)
        with jax.named_scope(f"d{n}_prodA"):
            product(n, 1 - core, lambda unit: pair_send.at[bounds[n] + unit])
            pair_copy(n).start()
        if n >= first:
            with jax.named_scope(f"d{n}_relay"):
                relay(n)
                if n - 2 in meets:
                    meet(n - 2)
        with jax.named_scope(f"d{n}_finish"):
            if finished < n:
                finish(n - 1)
                finished = n
        with jax.named_scope(f"d{n}_prodB"):
            product(n, core, lambda unit: pair_own.at[n % 2, unit])
        if n + 1 == count or chunks[n + 1][2] != wave:
            with jax.named_scope(f"d{n}_finish"):
                finish(n)
                finished = n + 1
        if n < first:
            with jax.named_scope(f"d{n}_relay"):
                relay(n)
    def free(those, which):
        for k in range(n_z - 1, 0, -1):
            for n in those:
                to = (z + k) % n_z

                @pl.when(held(n, to) & which(to))
                def _():
                    straight_copy(n, k).start()

    free(lasting, lambda to: to < z)
    with jax.named_scope("lastrelay"):
        for t in range(count, first + n_z + 2):
            relay(t)
        for n in meets:
            if n + 2 >= count:
                meet(n)
        free((count - 1,), lambda to: to > z)

    mine = slot_rows(z)

    def total_of(n, unit):
        if narrow[n]:
            short = own_tok // 2
            branch = z_send[unit, pl.ds(pl.multiple_of(z * short, short), short), :].astype(f32)
            for k in range(n_z - 1):
                branch = branch + z_pass[unit, k, :short, :].astype(f32)
            return jnp.concatenate([branch[:, :width // 2], branch[:, width // 2:]], axis=0)
        branch = z_send[unit, mine, :].astype(f32)
        if n < first:
            return branch + z_last[0, unit].astype(f32) + z_last[1, unit].astype(f32)
        for k in range(n_z - 1):
            branch = branch + z_pass[unit, k].astype(f32)
        return branch

    def settle(mask, top, parts):
        start = flip_all(fs, mask, dims) * rows + top
        to = pl.ds(pl.multiple_of(start, width), width)
        branch = jnp.concatenate(parts, axis=1) if len(parts) > 1 else parts[0]
        mixed[:, to] = (tok_in[:, to].astype(f32) + 0.5 * branch).astype(jnp.bfloat16)

    with jax.named_scope("lastwait"):
        spread = pl.ds(0, bounds[first])
        for side, end in ((0, 0), (1, n_z - 1)):
            @pl.when(z != end)
            def _():
                pltpu.make_async_remote_copy(
                    src_ref=z_last.at[side, spread], dst_ref=z_last.at[side, spread],
                    send_sem=z_sent.at[0], recv_sem=l_got.at[side],
                    device_id={"tp": sibling}, device_id_type=MESH,
                ).wait_recv()
    open_parts = {}
    for n, (blocks, _, _) in enumerate(chunks):
        with jax.named_scope(f"last{n}"):
            if n >= first:
                spread = pl.ds(bounds[n], units[n])
                tall = own_tok // 2 if narrow[n] else own_tok

                def came(many):
                    here = z_pass.at[spread, pl.ds(0, many), pl.ds(0, tall)]
                    pltpu.make_async_remote_copy(
                        src_ref=here, dst_ref=here, send_sem=z_sent.at[0], recv_sem=f_got.at[n - first],
                        device_id={"tp": sibling}, device_id_type=MESH,
                    ).wait_recv()

                if n not in meets:
                    came(n_z - 1)
                else:
                    edges = ((n_z - 1, n_z - 1), (0, 1))[:2 if n in low_meets else 1]
                    at_edge = (z == n_z - 1) | (z == 0) if n in low_meets else z == n_z - 1

                    @pl.when(jnp.logical_not(at_edge))
                    def _():
                        came(n_z - 1)

                    @pl.when(at_edge)
                    def _():
                        came(n_z - 2)
                    for edge, k in edges:
                        @pl.when(z == edge)
                        def _():
                            z_pass[spread, k - 1] = jnp.zeros((units[n], own_tok, width), jnp.bfloat16)
            sums = [total_of(n, unit) for unit in range(bounds[n], bounds[n + 1])]
            lane = 0
            for mask, top, tall in blocks:
                if tall < width:
                    key = (mask, top // width * width)
                    open_parts.setdefault(key, []).append(sums[0][:, lane:lane + tall])
                    lane += tall
                    if sum(piece.shape[1] for piece in open_parts[key]) == width:
                        settle(mask, key[1], open_parts.pop(key))
                    continue
                for at in range(0, tall, width):
                    settle(mask, top + at, [sums[lane // width]])
                    lane += width

    def sent(ref, sem):
        pltpu.make_async_remote_copy(
            src_ref=ref, dst_ref=ref, send_sem=sem, recv_sem=sem,
            device_id={"tp": sibling}, device_id_type=MESH,
        ).wait_send()

    whole = pl.ds(0, n_fs * rows // width)
    for w in range(3):
        sent(ready[w].at[pl.ds(0, every * rows), :], w_sent.at[w])
    sent(tok.at[pl.ds(0, (2 * n_z - 1) * own_tok), :], t_sent.at[0])
    sent(pair_send.at[whole], p_sent.at[0])
    sent(z_pass.at[whole], z_sent.at[0])


def store(*refs):
    count = len(refs) // 2
    done = refs[-1]
    copies = []
    for n in range(count):
        tall = refs[n].shape[0] // 2
        for h in range(2):
            at = pl.ds(h * tall, tall)
            copies.append(pltpu.make_async_copy(refs[n].at[at, :], refs[count + n].at[at, :], done.at[n, h]))
            copies[-1].start()
    for copy in copies:
        copy.wait()


def body(n_fs, n_tp, tokens, norm_gain, gate_master, up_master, down_master):
    own_tok, depth = tokens.shape
    rows, cols = gate_master.shape
    dims = n_fs.bit_length() - 1
    n_z = n_tp // 2
    half, total = n_z * own_tok, n_tp * own_tok
    part = rows // dims
    halves = part // 128 if part % 128 == 0 else 1
    late, other, width, chunks, first = plan(n_fs, dims, rows)
    count = sum(max(1, sum(tall for _, _, tall in blocks) // width) for blocks, _, _ in chunks)
    deal = sum(tall for _, _, tall in chunks[0][0]) // width
    steps = len(chunks)
    pieces = (1 if dims == 2 else dims) * ((n_fs - 1) * (1 + halves) + (n_fs - 2) * len(other) + len(late))
    bf16, f32 = jnp.bfloat16, jnp.float32
    dma = pltpu.SemaphoreType.DMA
    vmem = pl.BlockSpec(memory_space=pltpu.VMEM)
    hbm = pl.BlockSpec(memory_space=pltpu.HBM)
    operands = (tokens, norm_gain[None, :], gate_master, up_master, down_master)
    results = pl.pallas_call(
        functools.partial(kernel, n_fs, n_z, dims, halves, late, other, width, chunks, first),
        out_shape=(pltpu.VMEM((own_tok, depth), bf16),)
        + tuple(pltpu.VMEM((n_fs * rows, cols), bf16) for _ in range(3)),
        in_specs=[hbm] * 5,
        out_specs=(vmem,) * 4,
        scratch_shapes=[
            pltpu.VMEM((own_tok, depth), bf16),
            pltpu.VMEM((1, rows), f32),
            pltpu.VMEM((rows, 128), f32),
            pltpu.VMEM((3, rows, cols), f32),
            pltpu.VMEM((total, depth), bf16),
            pltpu.VMEM((total, 1), f32),
            pltpu.VMEM((total, cols), f32),
            pltpu.VMEM((total, cols), f32),
            pltpu.VMEM((total, cols), bf16),
            pltpu.VMEM((2, deal, half, width), f32),
            pltpu.VMEM((count, half, width), bf16),
            pltpu.VMEM((count, half, width), bf16),
            pltpu.VMEM((count, half, width), bf16),
            pltpu.VMEM((count, n_z - 1, own_tok, width), bf16),
            pltpu.VMEM((2, count, own_tok, width), bf16),
            dma((3,)), dma((pieces,)),
            dma((1,)), dma((n_z - 1,)), dma((1,)),
            dma((1,)), dma((steps + n_z,)),
            dma((1,)), dma((first, n_z - 1)), dma((2,)), dma((steps - first,)), dma((steps - first,)),
            dma((4 * dims + 3,)),
        ],
        compiler_params=pltpu.CompilerParams(
            collective_id=0, has_side_effects=True, vmem_limit_bytes=40 * 1024 * 1024
        ),
    )(*(pltpu.with_memory_space_constraint(value, pltpu.HBM) for value in operands))
    return pl.pallas_call(
        store,
        out_shape=tuple(jax.ShapeDtypeStruct(result.shape, result.dtype) for result in results),
        in_specs=[vmem] * 4,
        out_specs=(hbm,) * 4,
        scratch_shapes=[dma((4, 2))],
        compiler_params=pltpu.CompilerParams(vmem_limit_bytes=1024 * 1024),
    )(*(pltpu.with_memory_space_constraint(result, pltpu.VMEM) for result in results))


def solution(mesh):
    in_specs = (P(("fs", "tp"), None), P("fs"), P("fs", "tp"), P("fs", "tp"), P("fs", "tp"))
    out_specs = (P(("fs", "tp"), None), P(None, "tp"), P(None, "tp"), P(None, "tp"))
    step = functools.partial(body, mesh.shape["fs"], mesh.shape["tp"])
    return jax.shard_map(step, mesh=mesh, in_specs=in_specs, out_specs=out_specs, check_vma=False)
```

```python
import functools
import math

import jax
import jax.numpy as jnp
from jax import lax
from jax.experimental import pallas as pl
from jax.experimental.pallas import tpu as pltpu
from jax.sharding import PartitionSpec as P

MESH = pl.DeviceIdType.MESH
GATE, UP, DOWN = 0, 1, 2


def flip(index, bit):
    return index + bit - 2 * bit * ((index // bit) % 2)


def flip_all(index, mask, dims):
    for dim in range(dims):
        if mask >> dim & 1:
            index = flip(index, 1 << dim)
    return index


def span(bits):
    masks = [0]
    for bit in bits:
        masks += [mask | bit for mask in masks]
    return masks


def plan(n_fs, dims, rows):
    part = rows // dims
    last = n_fs - 1
    if dims != 2 or part % 128 or rows % 256:
        chunks = [([(mask, 0, rows)], [(p, 0, mask) for p in range(dims)], mask) for mask in range(n_fs)]
        return [part], [part], rows, chunks, last
    late, other = [64] * (part // 64), [128] * (part // 128)
    chunks = [([(0, at, 256)], [], 0) for at in range(0, rows, 256)]
    for step, owners in enumerate(([(1, 0), (2, 1)], [(2, 0), (1, 1)], [(last, 0), (last, 1)])):
        heights = late if step == 2 else other
        for h, tall in enumerate(heights):
            blocks = [(mask, p * part + sum(heights[:h]), tall) for mask, p in owners]
            chunks.append((blocks, [(p, h, mask) for mask, p in owners], (step, h)))
    return late, other, 128, chunks, next(n for n, chunk in enumerate(chunks) if chunk[2] == (1, len(other) - 1))


def kernel(
    n_fs, n_z, dims, halves, late, other, width, chunks, first,
    tok_hbm, gain_hbm, gate_hbm, up_hbm, down_hbm,
    mixed, gate, up, down,
    tok_in, gain_row, gain, masters, tok, scale, gate_acc, up_acc, hidden, pair_own, pair_send, pair_recv, z_send, z_pass, z_last,
    w_sent, w_got, t_sent, t_got, s_got, p_sent, p_got, z_sent, z_got, l_got, f_got, m_got, loaded,
):
    fs, tp = lax.axis_index("fs"), lax.axis_index("tp")
    z, core = tp // 2, tp % 2
    sibling = z * 2 + 1 - core
    rows, cols = gate_hbm.shape
    part = rows // dims
    own_tok = tok_in.shape[0]
    half = n_z * own_tok
    total = 2 * half
    ready = (gate, up, down)
    every = n_fs - 1

    def heights(w, mask):
        if w == DOWN:
            return late if mask == every else other
        many = (1, halves)[w]
        return [part // many] * many

    def cuts(w, mask):
        return len(heights(w, mask))

    loads = {}
    reads = [("gain", gain_hbm, gain_row)]
    for w, master in ((GATE, gate_hbm), (UP, up_hbm)):
        for p in range(dims):
            for i in range(2):
                mine = pl.ds(p * part + i * part // 2, part // 2)
                reads.append(((w, p, i), master.at[mine, :], masters.at[w, mine, :]))
    reads.append(("tok", tok_hbm, tok_in))
    reads.append(("down", down_hbm, masters.at[DOWN]))
    for n, (name, src, dst) in enumerate(reads):
        loads[name] = pltpu.make_async_copy(src, dst, loaded.at[n])

    def z_peer(k):
        return ((z + k) % n_z) * 2 + core

    for name, _, _ in reads[:1 + 2 * dims]:
        loads[name].start()
    barrier = pltpu.get_barrier_semaphore()
    for dim in range(dims):
        pl.semaphore_signal(barrier, 1, device_id={"fs": flip(fs, 1 << dim)}, device_id_type=MESH)
    for k in range(1, n_z):
        pl.semaphore_signal(barrier, 1, device_id={"tp": z_peer(k)}, device_id_type=MESH)
    pl.semaphore_signal(barrier, 1, device_id={"tp": sibling}, device_id_type=MESH)

    loads["gain"].wait()
    for n in range(rows // 128):
        line = gain_row[:, n * 128:(n + 1) * 128]
        gain[n * 128:(n + 1) * 128, :] = jnp.transpose(jnp.broadcast_to(line, (128, 128)))

    def block(w, owner, p, h, mask):
        tall, top = heights(w, mask)[h], sum(heights(w, mask)[:h])
        start = flip_all(fs, owner, dims) * rows + p * part + top
        return ready[w].at[pl.ds(pl.multiple_of(start, tall), tall), :]

    def order(p):
        return [1 << ((p + s) % dims) for s in range(dims)]

    arrivals = {
        (p, held | order(p)[stage]): stage
        for p in range(dims) for stage in range(dims) for held in span(order(p)[:stage])
    }
    arrived = set()

    def together(w, p, h, mask):
        if dims != 2:
            return [(p, mask)]
        return sorted([(p, mask), (1 - p, mask if mask == every else every - mask)])

    place = {}
    for w in (GATE, UP, DOWN):
        for p in range(dims):
            for mask in range(1, n_fs):
                for h in range(cuts(w, mask)):
                    place.setdefault((w, h, *together(w, p, h, mask)), len(place))

    def got(w, p, h, mask):
        return w_got.at[place[(w, h, *together(w, p, h, mask))]]

    def weight_copy(w, p, h, held, mask, stage):
        return pltpu.make_async_remote_copy(
            src_ref=block(w, held, p, h, mask), dst_ref=block(w, held, p, h, mask),
            send_sem=w_sent.at[w], recv_sem=got(w, p, h, mask),
            device_id={"fs": flip(fs, order(p)[stage])}, device_id_type=MESH,
        )

    def send(w, p, h, stage, held):
        weight_copy(w, p, h, held, held | order(p)[stage], stage).start()

    def need(w, p, h, mask, hold=False):
        if mask and (w, p, h, mask) not in arrived:
            pair = together(w, p, h, mask)
            tall = heights(w, mask)[h] * len(pair)
            here = ready[w].at[pl.ds(0, tall), :] if len(pair) > 1 else block(w, mask, p, h, mask)
            pltpu.make_async_remote_copy(
                src_ref=here, dst_ref=here, send_sem=w_sent.at[w], recv_sem=got(w, p, h, mask),
                device_id={"fs": flip(fs, 1)}, device_id_type=MESH,
            ).wait_recv()
            for p, mask in pair:
                arrived.add((w, p, h, mask))
                if not hold:
                    forward(w, p, h, mask)

    def forward(w, p, h, mask):
        for later in range(arrivals[p, mask] + 1, dims):
            top, finer = sum(heights(w, mask)[:h]), heights(w, mask | order(p)[later])
            for piece in range(len(finer)):
                if top <= sum(finer[:piece]) < top + heights(w, mask)[h]:
                    send(w, p, piece, later, mask)

    def relays(ws):
        for stage in range(dims - 1):
            for w in ws:
                for p in range(dims):
                    for held in span(order(p)[:stage]):
                        for h in range(cuts(w, held | order(p)[stage])):
                            need(w, p, h, held | order(p)[stage])

    def prepare(w, top, tall):
        mine = slice(top, top + tall)
        value = masters[w, mine, :]
        if w != DOWN:
            value = gain[mine, 0:1] * value
        ready[w][pl.ds(pl.multiple_of(fs * rows + top, tall), tall), :] = value.astype(jnp.bfloat16)

    short = part // 2
    for p in range(dims):
        for i in range(2):
            loads[GATE, p, i].wait()
            prepare(GATE, p * part + i * short, short)
            if p == 0 and i == 0:
                with jax.named_scope("barrier"):
                    pl.semaphore_wait(barrier, dims + n_z)
            at = gate.at[pl.ds(pl.multiple_of(fs * rows + p * part + i * short, short), short), :]
            pltpu.make_async_remote_copy(
                src_ref=at, dst_ref=at, send_sem=w_sent.at[GATE], recv_sem=got(GATE, p, 0, order(p)[0]),
                device_id={"fs": flip(fs, order(p)[0])}, device_id_type=MESH,
            ).start()
    for name, _, _ in reads[1 + 2 * dims:]:
        loads[name].start()
    for p in range(dims):
        for i in range(2):
            loads[UP, p, i].wait()
        prepare(UP, p * part, part)
        for h in range(cuts(UP, 0)):
            send(UP, p, h, 0, 0)

    def tok_rows(c, chip):
        start = (c * n_z + chip) * own_tok
        return tok.at[pl.ds(pl.multiple_of(start, own_tok), own_tok), :]

    def tok_z(k):
        return pltpu.make_async_remote_copy(
            src_ref=tok_in, dst_ref=tok_rows(core, z), send_sem=t_sent.at[0], recv_sem=t_got.at[k - 1],
            device_id={"tp": z_peer(k)}, device_id_type=MESH,
        )

    def tok_sibling(src, slot):
        return pltpu.make_async_remote_copy(
            src_ref=src, dst_ref=slot, send_sem=t_sent.at[0], recv_sem=s_got.at[0],
            device_id={"tp": sibling}, device_id_type=MESH,
        )

    loads["tok"].wait()
    for k in range(1, n_z):
        tok_z(k).start()
    tok_sibling(tok_in, tok_rows(core, z)).start()
    for w in (GATE, UP):
        for p in range(dims):
            for stage in range(1, dims):
                for h in range(cuts(w, 0)):
                    send(w, p, h, stage, 0)
    tok_rows(core, z)[...] = tok_in[...]
    loads["down"].wait()
    for p in range(dims):
        prepare(DOWN, p * part, part)

    @pl.when(z == 0)
    def _():
        z_last[0] = jnp.zeros(z_last.shape[1:], jnp.bfloat16)

    @pl.when(z == n_z - 1)
    def _():
        z_last[1] = jnp.zeros(z_last.shape[1:], jnp.bfloat16)

    with jax.named_scope("relays"):
        relays((GATE, UP))

    def send_down(turn, stages):
        @pl.when(core == turn)
        def _():
            for stage in stages:
                for h in range(max(cuts(DOWN, order(p)[stage]) for p in range(dims))):
                    for p in range(dims):
                        send(DOWN, p, h, stage, 0)

    split = dims == 2 and first > 4
    send_down(0, range(1) if split else range(dims))

    for k in range(1, n_z):
        slot = tok_rows(core, (z + n_z - k) % n_z)
        with jax.named_scope(f"tokwait{k}"):
            pltpu.make_async_remote_copy(
                src_ref=slot, dst_ref=slot, send_sem=t_sent.at[0], recv_sem=t_got.at[k - 1],
                device_id={"tp": z_peer(k)}, device_id_type=MESH,
            ).wait_recv()
        tok_sibling(slot, slot).start()
    rest = tok.at[pl.ds(pl.multiple_of((1 - core) * half, half), half), :]
    with jax.named_scope("tokpair"):
        pltpu.make_async_remote_copy(
            src_ref=rest, dst_ref=rest, send_sem=t_sent.at[0], recv_sem=s_got.at[0],
            device_id={"tp": sibling}, device_id_type=MESH,
        ).wait_recv()

    tile_m, tile_n = min(256, half), min(512, cols)
    across = cols // tile_n
    tile_s = min(64, total)
    f32 = jnp.float32

    @pl.loop(0, total // tile_s)
    def _(i):
        at = pl.ds(pl.multiple_of(i * tile_s, tile_s), tile_s)
        wide = tok[at, :].astype(f32)
        scale[at, :] = lax.rsqrt(jnp.mean(wide * wide, axis=1, keepdims=True) + 1e-06)

    def tiles(count, first, run):
        @pl.loop(0, (count // tile_m) * across)
        def _(i):
            at = pl.ds(pl.multiple_of(first + (i // across) * tile_m, tile_m), tile_m)
            run(at, pl.ds(pl.multiple_of((i % across) * tile_n, tile_n), tile_n))

    def deep(mask):
        return pl.ds(pl.multiple_of(flip_all(fs, mask, dims) * rows, rows), rows)

    def dot(x, w):
        return jnp.dot(x, w, preferred_element_type=f32)

    def piece_dot(at, to, h):
        if halves == 1:
            return dot(tok[at, deep(every)], up[deep(every), to])
        tall = part // halves
        owner = flip_all(fs, every, dims) * rows
        spots = [pl.ds(pl.multiple_of(owner + p * part + h * tall, tall), tall) for p in range(dims)]
        x = jnp.concatenate([tok[at, spot] for spot in spots], axis=1)
        return dot(x, jnp.concatenate([up[spot, to] for spot in spots], axis=0))

    for mask in range(every):
        for w in (GATE, UP):
            for p in range(dims):
                for h in range(cuts(w, mask)):
                    with jax.named_scope(f"early_need{mask}{w}{p}{h}"):
                        need(w, p, h, mask)

    def early(at, to):
        g, u = dot(tok[at, deep(0)], gate[deep(0), to]), dot(tok[at, deep(0)], up[deep(0), to])
        for mask in range(1, every):
            g = g + dot(tok[at, deep(mask)], gate[deep(mask), to])
            u = u + dot(tok[at, deep(mask)], up[deep(mask), to])
        gate_acc[at, to] = g
        up_acc[at, to] = u

    with jax.named_scope("early"):
        tiles(total, 0, early)

    for p in range(dims):
        with jax.named_scope(f"gate_need{p}"):
            need(GATE, p, 0, every)

    def gate_end(at, to):
        g = scale[at, :] * (gate_acc[at, to] + dot(tok[at, deep(every)], gate[deep(every), to]))
        gate_acc[at, to] = scale[at, :] * (g / (1.0 + jnp.exp(-g)))

    with jax.named_scope("gate_end"):
        tiles(total, 0, gate_end)

    for h in range(cuts(UP, every) - 1):
        for p in range(dims):
            with jax.named_scope(f"up_need{h}{p}"):
                need(UP, p, h, every)

        def up_more(at, to):
            up_acc[at, to] = up_acc[at, to] + piece_dot(at, to, h)

        with jax.named_scope(f"up_more{h}"):
            tiles(total, 0, up_more)

    for p in range(dims):
        with jax.named_scope(f"up_need{cuts(UP, every) - 1}{p}"):
            need(UP, p, cuts(UP, every) - 1, every)

    send_down(1, range(dims))

    def up_end(at, to):
        u = up_acc[at, to] + piece_dot(at, to, cuts(UP, every) - 1)
        hidden[at, to] = (gate_acc[at, to] * u).astype(jnp.bfloat16)

    spans = [sum(tall for _, _, tall in blocks) for blocks, _, _ in chunks]
    units = [max(1, wide // width) for wide in spans]
    narrow = [wide < width for wide in spans]
    bounds = [sum(units[:n]) for n in range(len(units) + 1)]
    count = len(chunks)

    def slot_rows(d):
        return pl.ds(pl.multiple_of(d * own_tok, own_tok), own_tok)

    def product(n, parity, out, slot=None):
        tile = own_tok if slot is not None else min(256, half)
        spots = []
        for mask, top, tall in chunks[n][0]:
            start = flip_all(fs, mask, dims) * rows + top
            spots.append(pl.ds(pl.multiple_of(start, math.gcd(tall, top) if top else tall), tall))

        def run(i):
            at = pl.ds(pl.multiple_of(i * tile, tile), tile)
            src = pl.ds(pl.multiple_of(parity * half + i * tile, tile), tile)
            w = [down[spot, :] for spot in spots]
            value = lax.dot_general(
                hidden[src, :], w[0] if len(w) == 1 else jnp.concatenate(w, axis=0),
                (((1,), (1,)), ((), ())), preferred_element_type=f32,
            )
            if narrow[n]:
                value = jnp.concatenate([
                    jnp.concatenate([value[r:r + own_tok // 2], value[r + own_tok // 2:r + own_tok]], axis=1)
                    for r in range(0, tile, own_tok)
                ], axis=0)
                at = pl.ds(pl.multiple_of(i * (tile // 2), tile // 2), tile // 2)
            for unit in range(units[n]):
                out(unit)[at, :] = value[:, unit * width:(unit + 1) * width].astype(out(unit).dtype)

        if slot is not None:
            run(slot)
        else:
            pl.loop(0, half // tile)(run)

    def pair_copy(n, i=None, slot=None):
        mine = pl.ds(bounds[n], units[n])
        at = (mine, pl.ds(0, half // 2 if narrow[n] else half)) if slot is None else (mine, slot_rows(slot))
        return pltpu.make_async_remote_copy(
            src_ref=pair_send.at[at], dst_ref=pair_recv.at[at],
            send_sem=p_sent.at[0], recv_sem=p_got.at[n if i is None else count + i],
            device_id={"tp": sibling}, device_id_type=MESH,
        )

    def passing(side, hops):
        return hops - 1 if side > 0 else n_z - 1 - hops

    deal = units[0]
    meets = range(first, count - 1 if n_z > 3 else first)
    low_meets = range(first, max(first, meets.stop - 1))
    lasting = range(max(first, count - 2), count)

    def chain_copy(n, side, hops):
        mine = pl.ds(n * deal, deal)
        if hops == 1:
            dst, got = z_last.at[(1 - side) // 2, mine], l_got.at[(1 - side) // 2]
        else:
            dst, got = z_pass.at[mine, passing(side, hops - 1)], z_got.at[n, passing(side, hops - 1)]
        to = jnp.clip(z + side, 0, n_z - 1)
        return pltpu.make_async_remote_copy(
            src_ref=z_send.at[mine, slot_rows(jnp.clip(z + side * hops, 0, n_z - 1)), :], dst_ref=dst,
            send_sem=z_sent.at[0], recv_sem=got,
            device_id={"tp": to * 2 + core}, device_id_type=MESH,
        )

    def straight_copy(n, k):
        mine = pl.ds(bounds[n], units[n])
        tall = own_tok // 2 if narrow[n] else own_tok
        at = pl.ds(pl.multiple_of(((z + k) % n_z) * tall, tall), tall)
        return pltpu.make_async_remote_copy(
            src_ref=z_send.at[mine, at, :], dst_ref=z_pass.at[mine, k - 1, pl.ds(0, tall)],
            send_sem=z_sent.at[0], recv_sem=f_got.at[n - first],
            device_id={"tp": z_peer(k)}, device_id_type=MESH,
        )

    def meet_copy(n, to):
        mine = pl.ds(bounds[n], units[n])
        return pltpu.make_async_remote_copy(
            src_ref=z_send.at[mine, slot_rows(to), :], dst_ref=z_last.at[0, mine],
            send_sem=z_sent.at[0], recv_sem=m_got.at[n - first],
            device_id={"tp": jnp.where(z == 0, 1, n_z - 2) * 2 + core}, device_id_type=MESH,
        )

    def meet(n):
        for at, to in ((1, n_z - 1), (n_z - 2, 0))[:2 if n in low_meets else 1]:
            @pl.when(z == at)
            def _():
                meet_copy(n, to).wait_recv()
                for unit in range(bounds[n], bounds[n + 1]):
                    rest = slice(to * own_tok, (to + 1) * own_tok)
                    both = z_send[unit, rest, :].astype(f32) + z_last[0, unit].astype(f32)
                    z_send[unit, rest, :] = both.astype(jnp.bfloat16)
                straight_copy(n, (to - at) % n_z).start()

    def held(n, to):
        inner = (z > 0) & (z < n_z - 1)
        low = (to > 0) & (to < z) if n in lasting else to < 0
        return low | (inner & (to == z + 1)) if n == count - 1 else low

    def at_ends(run):
        for side, end in ((1, 0), (-1, n_z - 1)):
            @pl.when(z == end)
            def _():
                run(side)

    def finish(n):
        pair_copy(n).wait_recv()
        for unit in range(units[n]):
            at, rest = bounds[n] + unit, slice(0, half // 2 if narrow[n] else half)
            z_send[at, rest, :] = (pair_own[n % 2, unit, rest, :] + pair_recv[at, rest, :].astype(f32)).astype(jnp.bfloat16)
        if n >= first:
            for k in range(n_z - 1, 0, -1):
                hop = jnp.where(z < n_z // 2, k, n_z - k)
                to = (z + hop) % n_z
                later = held(n, to)
                if n in meets:
                    over, waits = (z == 0) & (to == n_z - 1), (z == 1) & (to == n_z - 1)
                    if n in low_meets:
                        over, waits = over | ((z == n_z - 1) & (to == 0)), waits | ((z == n_z - 2) & (to == 0))

                    @pl.when(over)
                    def _():
                        meet_copy(n, to).start()

                    later = later | over | waits

                @pl.when(jnp.logical_not(later))
                def _():
                    straight_copy(n, hop).start()
        else:
            at_ends(lambda side: [chain_copy(n, side, hops).start() for hops in range(n_z - 1, 0, -1)])

    def pass_on(n, depth, side):
        mine = pl.ds(n * deal, deal)
        for hops in range(n_z - 2, 0, -1):
            @pl.when(depth + hops < n_z)
            def _():
                at = passing(side, hops)
                pltpu.make_async_remote_copy(
                    src_ref=z_pass.at[mine, at], dst_ref=z_pass.at[mine, at],
                    send_sem=z_sent.at[0], recv_sem=z_got.at[n, at],
                    device_id={"tp": sibling}, device_id_type=MESH,
                ).wait_recv()
                to = slot_rows(jnp.clip(z + side * hops, 0, n_z - 1))
                both = z_send[mine, to, :].astype(f32) + z_pass[mine, at].astype(f32)
                z_send[mine, to, :] = both.astype(jnp.bfloat16)
                chain_copy(n, side, hops).start()

    def relay(t):
        for side in (1, -1):
            depth = z if side > 0 else n_z - 1 - z
            inner = (depth > 0) & (depth < n_z - 1)
            for later in (1, 0):
                n = t - depth - later
                far = (depth > 1) * 1
                lag = (n < 2) * 1 + (n == first - 1) * far
                turn = inner & (n >= 0) & (n < first) & (lag == later)

                @pl.when(turn)
                def _():
                    pass_on(n, depth, side)

    def open_up():
        slots = [jnp.where(z < n_z // 2, n_z - 1 - i, i) for i in range(n_z)]

        def half_of(parity, slot):
            first_row = parity * half + slot * own_tok
            at = pl.ds(pl.multiple_of(first_row, own_tok), own_tok)
            for j in range(across):
                up_end(at, slice(j * tile_n, (j + 1) * tile_n))

        def away(i):
            half_of(1 - core, slots[i])
            product(0, 1 - core, lambda unit: pair_send.at[unit], slots[i])
            pair_copy(0, i, slots[i]).start()

        def close(i):
            half_of(core, slots[i])
            product(0, core, lambda unit: pair_own.at[0, unit], slots[i])
            pair_copy(0, i, slots[i]).wait_recv()
            here = slot_rows(slots[i])
            for unit in range(deal):
                own = pair_own[0, unit, here, :] + pair_recv[unit, here, :].astype(f32)
                z_send[unit, here, :] = own.astype(jnp.bfloat16)
            if i < n_z - 1:
                at_ends(lambda side: chain_copy(0, side, n_z - 1 - i).start())

        for i in range(n_z):
            with jax.named_scope(f"away{i}"):
                away(i)
            if i:
                with jax.named_scope(f"close{i - 1}"):
                    close(i - 1)
        with jax.named_scope(f"close{n_z - 1}"):
            close(n_z - 1)

    with jax.named_scope("open"):
        open_up()
    finished = 1
    for n, (blocks, needs, wave) in enumerate(chunks):
        if n == 0:
            continue
        for p, h, mask in needs:
            with jax.named_scope(f"d{n}_need"):
                need(DOWN, p, h, mask, hold=split and n in (2, 3))
        if split and n == 3:
            for p, h, mask in chunks[2][1] + chunks[3][1]:
                forward(DOWN, p, h, mask)
        with jax.named_scope(f"d{n}_prodA"):
            product(n, 1 - core, lambda unit: pair_send.at[bounds[n] + unit])
            pair_copy(n).start()
        if n >= first:
            with jax.named_scope(f"d{n}_relay"):
                relay(n)
                if n - 2 in meets:
                    meet(n - 2)
        with jax.named_scope(f"d{n}_finish"):
            if finished < n:
                finish(n - 1)
                finished = n
        with jax.named_scope(f"d{n}_prodB"):
            product(n, core, lambda unit: pair_own.at[n % 2, unit])
        if split and n == 2:
            send_down(0, range(1, dims))
        if n + 1 == count or chunks[n + 1][2] != wave:
            with jax.named_scope(f"d{n}_finish"):
                finish(n)
                finished = n + 1
        if n < first:
            with jax.named_scope(f"d{n}_relay"):
                relay(n)
    def free(those, which):
        for k in range(n_z - 1, 0, -1):
            for n in those:
                to = (z + k) % n_z

                @pl.when(held(n, to) & which(to))
                def _():
                    straight_copy(n, k).start()

    free(lasting, lambda to: to < z)
    with jax.named_scope("lastrelay"):
        for t in range(count, first + n_z + 2):
            relay(t)
        for n in meets:
            if n + 2 >= count:
                meet(n)
        free((count - 1,), lambda to: to > z)

    mine = slot_rows(z)

    def total_of(n, unit):
        if narrow[n]:
            short = own_tok // 2
            branch = z_send[unit, pl.ds(pl.multiple_of(z * short, short), short), :].astype(f32)
            for k in range(n_z - 1):
                branch = branch + z_pass[unit, k, :short, :].astype(f32)
            return jnp.concatenate([branch[:, :width // 2], branch[:, width // 2:]], axis=0)
        branch = z_send[unit, mine, :].astype(f32)
        if n < first:
            return branch + z_last[0, unit].astype(f32) + z_last[1, unit].astype(f32)
        for k in range(n_z - 1):
            branch = branch + z_pass[unit, k].astype(f32)
        return branch

    def settle(mask, top, parts):
        start = flip_all(fs, mask, dims) * rows + top
        to = pl.ds(pl.multiple_of(start, width), width)
        branch = jnp.concatenate(parts, axis=1) if len(parts) > 1 else parts[0]
        mixed[:, to] = (tok_in[:, to].astype(f32) + 0.5 * branch).astype(jnp.bfloat16)

    with jax.named_scope("lastwait"):
        spread = pl.ds(0, bounds[first])
        for side, end in ((0, 0), (1, n_z - 1)):
            @pl.when(z != end)
            def _():
                pltpu.make_async_remote_copy(
                    src_ref=z_last.at[side, spread], dst_ref=z_last.at[side, spread],
                    send_sem=z_sent.at[0], recv_sem=l_got.at[side],
                    device_id={"tp": sibling}, device_id_type=MESH,
                ).wait_recv()
    open_parts = {}
    for n, (blocks, _, _) in enumerate(chunks):
        with jax.named_scope(f"last{n}"):
            if n >= first:
                spread = pl.ds(bounds[n], units[n])
                tall = own_tok // 2 if narrow[n] else own_tok

                def came(many):
                    here = z_pass.at[spread, pl.ds(0, many), pl.ds(0, tall)]
                    pltpu.make_async_remote_copy(
                        src_ref=here, dst_ref=here, send_sem=z_sent.at[0], recv_sem=f_got.at[n - first],
                        device_id={"tp": sibling}, device_id_type=MESH,
                    ).wait_recv()

                if n not in meets:
                    came(n_z - 1)
                else:
                    edges = ((n_z - 1, n_z - 1), (0, 1))[:2 if n in low_meets else 1]
                    at_edge = (z == n_z - 1) | (z == 0) if n in low_meets else z == n_z - 1

                    @pl.when(jnp.logical_not(at_edge))
                    def _():
                        came(n_z - 1)

                    @pl.when(at_edge)
                    def _():
                        came(n_z - 2)
                    for edge, k in edges:
                        @pl.when(z == edge)
                        def _():
                            z_pass[spread, k - 1] = jnp.zeros((units[n], own_tok, width), jnp.bfloat16)
            sums = [total_of(n, unit) for unit in range(bounds[n], bounds[n + 1])]
            lane = 0
            for mask, top, tall in blocks:
                if tall < width:
                    key = (mask, top // width * width)
                    open_parts.setdefault(key, []).append(sums[0][:, lane:lane + tall])
                    lane += tall
                    if sum(piece.shape[1] for piece in open_parts[key]) == width:
                        settle(mask, key[1], open_parts.pop(key))
                    continue
                for at in range(0, tall, width):
                    settle(mask, top + at, [sums[lane // width]])
                    lane += width

    def sent(ref, sem):
        pltpu.make_async_remote_copy(
            src_ref=ref, dst_ref=ref, send_sem=sem, recv_sem=sem,
            device_id={"tp": sibling}, device_id_type=MESH,
        ).wait_send()

    whole = pl.ds(0, n_fs * rows // width)
    for w in range(3):
        sent(ready[w].at[pl.ds(0, every * rows), :], w_sent.at[w])
    sent(tok.at[pl.ds(0, (2 * n_z - 1) * own_tok), :], t_sent.at[0])
    sent(pair_send.at[whole], p_sent.at[0])
    sent(z_pass.at[whole], z_sent.at[0])


def store(*refs):
    count = len(refs) // 2
    done = refs[-1]
    copies = []
    for n in range(count):
        tall = refs[n].shape[0] // 2
        for h in range(2):
            at = pl.ds(h * tall, tall)
            copies.append(pltpu.make_async_copy(refs[n].at[at, :], refs[count + n].at[at, :], done.at[n, h]))
            copies[-1].start()
    for copy in copies:
        copy.wait()


def body(n_fs, n_tp, tokens, norm_gain, gate_master, up_master, down_master):
    own_tok, depth = tokens.shape
    rows, cols = gate_master.shape
    dims = n_fs.bit_length() - 1
    n_z = n_tp // 2
    half, total = n_z * own_tok, n_tp * own_tok
    part = rows // dims
    halves = part // 128 if part % 128 == 0 else 1
    late, other, width, chunks, first = plan(n_fs, dims, rows)
    count = sum(max(1, sum(tall for _, _, tall in blocks) // width) for blocks, _, _ in chunks)
    deal = sum(tall for _, _, tall in chunks[0][0]) // width
    steps = len(chunks)
    pieces = (1 if dims == 2 else dims) * ((n_fs - 1) * (1 + halves) + (n_fs - 2) * len(other) + len(late))
    bf16, f32 = jnp.bfloat16, jnp.float32
    dma = pltpu.SemaphoreType.DMA
    vmem = pl.BlockSpec(memory_space=pltpu.VMEM)
    hbm = pl.BlockSpec(memory_space=pltpu.HBM)
    operands = (tokens, norm_gain[None, :], gate_master, up_master, down_master)
    results = pl.pallas_call(
        functools.partial(kernel, n_fs, n_z, dims, halves, late, other, width, chunks, first),
        out_shape=(pltpu.VMEM((own_tok, depth), bf16),)
        + tuple(pltpu.VMEM((n_fs * rows, cols), bf16) for _ in range(3)),
        in_specs=[hbm] * 5,
        out_specs=(vmem,) * 4,
        scratch_shapes=[
            pltpu.VMEM((own_tok, depth), bf16),
            pltpu.VMEM((1, rows), f32),
            pltpu.VMEM((rows, 128), f32),
            pltpu.VMEM((3, rows, cols), f32),
            pltpu.VMEM((total, depth), bf16),
            pltpu.VMEM((total, 1), f32),
            pltpu.VMEM((total, cols), f32),
            pltpu.VMEM((total, cols), f32),
            pltpu.VMEM((total, cols), bf16),
            pltpu.VMEM((2, deal, half, width), f32),
            pltpu.VMEM((count, half, width), bf16),
            pltpu.VMEM((count, half, width), bf16),
            pltpu.VMEM((count, half, width), bf16),
            pltpu.VMEM((count, n_z - 1, own_tok, width), bf16),
            pltpu.VMEM((2, count, own_tok, width), bf16),
            dma((3,)), dma((pieces,)),
            dma((1,)), dma((n_z - 1,)), dma((1,)),
            dma((1,)), dma((steps + n_z,)),
            dma((1,)), dma((first, n_z - 1)), dma((2,)), dma((steps - first,)), dma((steps - first,)),
            dma((4 * dims + 3,)),
        ],
        compiler_params=pltpu.CompilerParams(
            collective_id=0, has_side_effects=True, vmem_limit_bytes=40 * 1024 * 1024
        ),
    )(*(pltpu.with_memory_space_constraint(value, pltpu.HBM) for value in operands))
    return pl.pallas_call(
        store,
        out_shape=tuple(jax.ShapeDtypeStruct(result.shape, result.dtype) for result in results),
        in_specs=[vmem] * 4,
        out_specs=(hbm,) * 4,
        scratch_shapes=[dma((4, 2))],
        compiler_params=pltpu.CompilerParams(vmem_limit_bytes=1024 * 1024),
    )(*(pltpu.with_memory_space_constraint(result, pltpu.VMEM) for result in results))


def solution(mesh):
    in_specs = (P(("fs", "tp"), None), P("fs"), P("fs", "tp"), P("fs", "tp"), P("fs", "tp"))
    out_specs = (P(("fs", "tp"), None), P(None, "tp"), P(None, "tp"), P(None, "tp"))
    step = functools.partial(body, mesh.shape["fs"], mesh.shape["tp"])
    return jax.shard_map(step, mesh=mesh, in_specs=in_specs, out_specs=out_specs, check_vma=False)
```
